512 devices in a mesh: grp: 2 (over y), sp: 32 (over z), tp: 8 (over x, core).
Axes of the slice: x: 4, y: 2, z: 32, core: 2. Of those that a mesh axis runs over, the one named last changes fastest.
The devices are a block of a 4x8x32 slice.
Arguments:
- queries: bfloat16 [32768, 1024], P(('grp', 'sp'), 'tp'), parts along dimension 0, may hold values from -6 to 6
- memory_keys: bfloat16 [32768, 1024], P(('grp', 'sp'), 'tp'), parts along dimension 0, may hold values from -6 to 6
- memory_values: bfloat16 [32768, 1024], P(('grp', 'sp'), 'tp'), parts along dimension 0, may hold values from -6 to 6
- output_preactivation: bfloat16 [32768, 1024], P(('grp', 'sp'), 'tp'), parts along dimension 0, may hold values from -12 to 12
- input_preactivation: float32 [8, 32768], P('tp', ('grp', 'sp')), parts along dimension 1, may hold values from -6 to 140
- forget_preactivation: float32 [8, 32768], P('tp', ('grp', 'sp')), parts along dimension 1, as said below
- extra_forget_terms: float32 [8, 32768], P('tp', ('grp', 'sp')), parts along dimension 1, may hold values from -1 to 0, as said below
- head_norm_gain: float32 [128], replicated, may hold values from 0.1 to 1.9
- output_projection_matrix: bfloat16 [1024, 2048], P('tp'), may hold values from -0.1875 to 0.1875
- residual: bfloat16 [32768, 2048], P(('grp', 'sp', 'tp')), parts along dimension 0, may hold values from -6 to 6
- feedforward_norm_gain: float32 [2048], replicated, may hold values from 0.1 to 1.9
- feedforward_up_matrix: bfloat16 [2048, 8192], P('sp', 'tp'), may hold values from -0.125 to 0.125
- feedforward_down_matrix: bfloat16 [8192, 2048], P('tp', 'sp'), may hold values from -0.0625 to 0.0625
Outputs:
- layer_out: bfloat16 [32768, 2048], P(('grp', 'sp', 'tp')), parts along dimension 0
The draws below stay inside these ranges and needn't reach their ends.
There are 2 independent parts, one for each index of `grp`. The reference program is written for one: setup_inputs(seed, part) draws one part's arguments, and reference() takes and returns one part's arrays. A program takes and returns all parts, laid end to end along the dimension named above; an argument that names none is the same for every part. Nothing has to cross between parts.
Inputs may be any that keep to these rules, and one draw needn't show every extreme that they name: `forget_preactivation`: forget gate pre-activations. `extra_forget_terms`: extra log forget terms, zero at most positions.
All inputs are finite; a program needn't handle non-finite values.
Results may differ from the reference program's by a relative error of at most 0.018.
Values may be sent and summed in bfloat16 or wider, within the bound.
No kernel may reach another device: no remote copies, remote signals or barrier semaphores. Data moves between devices by JAX's collectives and lax.ppermute only.
A program may use at most 64 MiB of HBM per device.

```python
import math
import jax
import jax.numpy as jnp
from jax import lax

D = 2048
FF = 8192
H = 8
DH = 128
BLOCK = 128
TOK_DEV = 512
M_WIDTH = 1024
SEQ = 16384
N_TP = 8


def draw_input_preactivation(key, part):
    draws = jax.random.split(jax.random.fold_in(key, 11), 1)
    values = jnp.clip(jax.random.normal(draws[0], (H, SEQ), jnp.float32), -6.0, 6.0)
    return values


def draw_forget_preactivation(key, part):
    draws = jax.random.split(jax.random.fold_in(key, 23), 3)
    order = jax.random.permutation(draws[0], H)
    slowly = order < H // 2
    center = jnp.where(slowly, math.log(2.5 * SEQ), 4.0).astype(jnp.float32)
    shifts = jax.random.uniform(draws[1], (H, SEQ // TOK_DEV, 1), jnp.float32, -0.7, 0.7)
    shifts = jnp.broadcast_to(shifts, (H, SEQ // TOK_DEV, TOK_DEV)).reshape(H, SEQ)
    jitter = jax.random.uniform(draws[2], (H, SEQ), jnp.float32, -1.0, 1.0)
    return center[:, None] + shifts + jitter


def draw_extra_forget_terms(key, part):
    draws = jax.random.split(jax.random.fold_in(key, 37), 2)
    quarter = SEQ // 4
    spots = jnp.arange(4)[None, :] * quarter + jax.random.randint(draws[0], (H, 4), 0, quarter)
    depths = jnp.log(jax.random.uniform(draws[1], (H, 4), jnp.float32, 0.5, 0.8))
    hits = jnp.arange(SEQ)[None, None, :] == spots[:, :, None]
    return jnp.sum(jnp.where(hits, depths[:, :, None], 0.0), axis=1)


def steps_of(stream_key, extent, cuts, low, top_value):
    gain, own = 1.0, jax.random.fold_in(stream_key, 6)
    for position, shards_of in cuts:
        steps = jnp.exp(jax.random.uniform(jax.random.fold_in(own, position), (shards_of,), jnp.float32, low / len(cuts), top_value / len(cuts)))
        gain = gain * jnp.repeat(steps, extent[position] // shards_of).reshape([-1 if axis == position else 1 for axis in range(len(extent))])
    return gain


def scatter_about(rng, shape, scale, reach, cuts=(), held_as=jnp.bfloat16):
    result = jax.random.normal(rng, shape, jnp.float32) * scale
    if len(cuts) > 0:
        result = steps_of(rng, shape, cuts, -0.22, 0.18) * result
    return jnp.clip(result, min=-reach, max=reach).astype(held_as)


def setup_inputs(seed: int = 0, part: int = 0) -> dict:
    key_of = jax.random.split(jax.random.key(seed), 14)
    part_splits = jax.random.split(jax.random.fold_in(key_of[13], part), 14)
    return {
        "queries": scatter_about(part_splits[0], (SEQ, M_WIDTH), 1.0, 6.0, ((0, 32), (1, 8))),
        "memory_keys": scatter_about(part_splits[1], (SEQ, M_WIDTH), 1.0, 6.0, ((0, 32), (1, 8))),
        "memory_values": scatter_about(part_splits[2], (SEQ, M_WIDTH), 1.0, 6.0, ((0, 32), (1, 8))),
        "output_preactivation": scatter_about(part_splits[3], (SEQ, M_WIDTH), 2.0, 12.0, ((0, 32), (1, 8))),
        "input_preactivation": draw_input_preactivation(jax.random.fold_in(jax.random.fold_in(key_of[13], part), 71), part),
        "forget_preactivation": draw_forget_preactivation(jax.random.fold_in(jax.random.fold_in(key_of[13], part), 71), part),
        "extra_forget_terms": draw_extra_forget_terms(jax.random.fold_in(jax.random.fold_in(key_of[13], part), 71), part),
        "head_norm_gain": jnp.clip(1.0 + 0.18 * jax.random.normal(key_of[7], (DH,), jnp.float32), 0.1, 1.9),
        "output_projection_matrix": scatter_about(key_of[8], (M_WIDTH, D), M_WIDTH ** -0.5, 0.1875, ((0, 8),)),
        "residual": scatter_about(part_splits[9], (SEQ, D), 1.0, 6.0, ((0, 256),)),
        "feedforward_norm_gain": jnp.clip(1.0 + 0.18 * jax.random.normal(key_of[10], (D,), jnp.float32), 0.1, 1.9),
        "feedforward_up_matrix": scatter_about(key_of[11], (D, FF), D ** -0.5, 0.125, ((0, 32), (1, 8))),
        "feedforward_down_matrix": scatter_about(key_of[12], (FF, D), FF ** -0.5, 0.0625, ((0, 8), (1, 32))),
    }


neg_big = -1e+30
norm_eps = 1e-06
highest = lax.Precision.HIGHEST

def rms_norm(tensor, gain_vec):
    mean_sq = lax.optimization_barrier(jnp.mean(tensor * tensor, axis=-1, keepdims=True))
    return tensor * lax.rsqrt(mean_sq + norm_eps) * gain_vec

def memory_cell(queries, memory_keys, memory_values, input_preactivation, forget_logarithm):
    blocks = SEQ // BLOCK

    def to_blocks(tensor):
        return jnp.moveaxis(tensor.reshape((H, blocks, BLOCK) + tensor.shape[2:]), 1, 0)
    causal = jnp.arange(BLOCK)[:, None] >= jnp.arange(BLOCK)[None, :]

    def advance(state_now, pieces):
        memory, stab_max = state_now
        query_blk, key_blk, val_blk, gate_blk, fgt_blk = pieces
        decay_logarithm = jnp.cumsum(fgt_blk, axis=-1)
        log_weight = decay_logarithm[:, :, None] - decay_logarithm[:, None, :] + gate_blk[:, None, :]
        log_weight = jnp.where(causal, log_weight, neg_big)
        carry_log = decay_logarithm + stab_max[:, None]
        row_max = jnp.maximum(lax.optimization_barrier(jnp.max(log_weight, axis=-1)), carry_log)
        scores = jnp.einsum('htd,hsd->hts', query_blk, key_blk, precision=highest) * jnp.exp(log_weight - row_max[..., None])
        carry_scale = jnp.exp(carry_log - row_max)
        hidden = jnp.einsum('hts,hsv->htv', scores, val_blk, precision=highest)
        hidden = hidden + carry_scale[..., None] * jnp.einsum('hvk,htk->htv', memory, query_blk, precision=highest)
        block_total = decay_logarithm[:, -1]
        tail_log = block_total[:, None] - decay_logarithm + gate_blk
        new_max = jnp.maximum(block_total + stab_max, lax.optimization_barrier(jnp.max(tail_log, axis=-1)))
        weights = jnp.exp(tail_log - new_max[:, None])
        carry_decay = jnp.exp(block_total + stab_max - new_max)
        memory = carry_decay[:, None, None] * memory + jnp.einsum('hs,hsv,hsk->hvk', weights, val_blk, key_blk, precision=highest)
        return ((memory, new_max), hidden)
    start_state = (jnp.zeros((H, DH, DH), jnp.float32), jnp.zeros((H,), jnp.float32))
    pieces = (to_blocks(queries), to_blocks(memory_keys), to_blocks(memory_values), to_blocks(input_preactivation), to_blocks(forget_logarithm))
    _, results = lax.scan(advance, start_state, pieces)
    return jnp.moveaxis(results, 0, 1).reshape(H, SEQ, DH)

def to_heads(tensor):
    return tensor.astype(jnp.float32).reshape(SEQ, H, DH).transpose(1, 0, 2)

def reference(queries, memory_keys, memory_values, output_preactivation, input_preactivation, forget_preactivation, extra_forget_terms, head_norm_gain, output_projection_matrix, residual, feedforward_norm_gain, feedforward_up_matrix, feedforward_down_matrix):
    forget_logarithm = jax.nn.log_sigmoid(forget_preactivation) + extra_forget_terms
    hidden = memory_cell(to_heads(queries), to_heads(memory_keys) * DH ** (-0.5), to_heads(memory_values), input_preactivation, forget_logarithm)
    hidden = hidden.transpose(1, 0, 2)
    gated = rms_norm(hidden, head_norm_gain) * jax.nn.sigmoid(output_preactivation.astype(jnp.float32).reshape(SEQ, H, DH))
    mixed = gated.reshape(SEQ, H * DH).astype(jnp.bfloat16)
    width_tp = H * DH // N_TP
    branch = jnp.zeros((SEQ, D), jnp.float32)
    for group_idx in range(N_TP):
        lower_col = group_idx * width_tp
        partial_value = jnp.dot(mixed[:, lower_col:lower_col + width_tp], output_projection_matrix[lower_col:lower_col + width_tp], preferred_element_type=jnp.float32)
        branch = branch + lax.optimization_barrier(partial_value.astype(jnp.bfloat16)).astype(jnp.float32)
    mid_state = (residual.astype(jnp.float32) + branch).astype(jnp.bfloat16)
    normed = rms_norm(mid_state.astype(jnp.float32), feedforward_norm_gain).astype(jnp.bfloat16)
    ff_tp = FF // N_TP
    mlp_sum = jnp.zeros((SEQ, D), jnp.float32)
    for group_idx in range(N_TP):
        lower_col = group_idx * ff_tp
        upward = jnp.dot(normed, feedforward_up_matrix[:, lower_col:lower_col + ff_tp], preferred_element_type=jnp.float32)
        active = jnp.square(jax.nn.relu(upward)).astype(jnp.bfloat16)
        partial_value = jnp.dot(active, feedforward_down_matrix[lower_col:lower_col + ff_tp], preferred_element_type=jnp.float32)
        mlp_sum = mlp_sum + lax.optimization_barrier(partial_value.astype(jnp.bfloat16)).astype(jnp.float32)
    return (mid_state.astype(jnp.float32) + mlp_sum).astype(jnp.bfloat16)
```

```python
import jax
import jax.numpy as jnp
from jax import lax
from jax.sharding import PartitionSpec as P

BLOCK = 128


neg_big = -1e30
norm_eps = 1e-06
highest = lax.Precision.HIGHEST


def turned_gather(arrays, axis, dims):
    turned = [jnp.moveaxis(a, dim, 0) for a, dim in zip(arrays, dims)]
    both = jnp.concatenate([t.reshape(len(t), -1) for t in turned], axis=1)
    filled, at, outs = (lax.all_gather(both, axis, axis=0, tiled=True), 0, [])
    for t, dim in zip(turned, dims):
        piece = filled[:, at : at + t[0].size].reshape(-1, *t.shape[1:])
        outs.append(jnp.moveaxis(piece, 0, dim))
        at += t[0].size
    return tuple(outs)


def shifted_on(x, axis, distance):
    length = lax.axis_size(axis)
    return lax.ppermute(x, axis, [(k, k + distance) for k in range(length - distance)])


def packed(state):
    total, top, memory = state
    scalars = jnp.stack([total, top], axis=1)
    row = jnp.pad(scalars, ((0, 0), (0, memory.shape[-1] - 2)))
    return jnp.concatenate([memory, jnp.broadcast_to(row[:, None], (*row.shape[:1], 8, row.shape[1]))], axis=1)


def unpacked(both, head_dim, present):
    top = jnp.where(present, both[:, head_dim, 1], neg_big)
    return (both[:, head_dim, 0], top, both[:, :head_dim])


def prefix_by_doubling(part, axis, combine):
    place = lax.axis_index(axis)
    length = lax.axis_size(axis)
    head_dim = part[2].shape[-1]
    window, earlier, distance = (part, None, 1)
    while distance < length:
        found = unpacked(shifted_on(packed(window), axis, distance), head_dim, place >= distance)
        earlier = found if earlier is None else combine(found, earlier)
        window = combine(found, window)
        distance *= 2
    return earlier


def cut_along(x, dim, length):
    before, after = (x.shape[:dim], x.shape[dim + 1 :])
    return jnp.moveaxis(x.reshape(*before, length, -1, *after), dim, 0)


def sum_at_owner(x, axis, dim):
    length = lax.axis_size(axis)
    blocks = lax.all_to_all(cut_along(x, dim, length), axis, 0, 0, tiled=True)
    return jnp.sum(blocks.astype(jnp.float32), axis=0)


def laid_out(blocks, dim):
    blocks = jnp.moveaxis(blocks, 0, dim)
    lengths = blocks.shape
    return blocks.reshape(*lengths[:dim], lengths[dim] * lengths[dim + 1], *lengths[dim + 2 :])


def copy_for_each(x, axis):
    copies = jnp.broadcast_to(x, (lax.axis_size(axis), *x.shape))
    return lax.all_to_all(copies, axis, split_axis=0, concat_axis=0, tiled=True)


def gather_directly(x, axis, dim):
    return laid_out(copy_for_each(x, axis), dim)


def rms_norm(tensor, gain_vec):
    mean_sq = jnp.mean(tensor * tensor, axis=-1, keepdims=True)
    return tensor * lax.rsqrt(mean_sq + norm_eps) * gain_vec


def combine(earlier, later):
    total_e, max_e, memory_e = earlier
    total_l, max_l, memory_l = later
    carried = total_l + max_e
    new_max = jnp.maximum(carried, max_l)
    old_part = jnp.exp(carried - new_max)
    new_part = jnp.exp(max_l - new_max)
    return (
        total_e + total_l,
        new_max,
        old_part[..., None, None] * memory_e + new_part[..., None, None] * memory_l,
    )


def block_summary(key_blk, val_blk, gate_blk, decay_logarithm):
    block_total = decay_logarithm[..., -1]
    tail_log = block_total[..., None] - decay_logarithm + gate_blk
    tail_max = jnp.max(tail_log, axis=-1)
    weights = jnp.exp(tail_log - tail_max[..., None])
    memory = jnp.einsum("bhsv,bhsk->bhvk", weights[..., None] * val_blk, key_blk, precision=highest)
    return (block_total, tail_max, memory)


def shards(
    queries,
    memory_keys,
    memory_values,
    output_preactivation,
    input_preactivation,
    forget_preactivation,
    extra_forget_terms,
    head_norm_gain,
    output_projection_matrix,
    residual,
    feedforward_norm_gain,
    feedforward_up_matrix,
    feedforward_down_matrix,
):
    tok_count = queries.shape[0]
    head_count = input_preactivation.shape[0]
    head_dim = queries.shape[1] // head_count
    block_len = BLOCK
    block_count = tok_count // block_len
    whole_up, whole_down = turned_gather(
        (feedforward_up_matrix, feedforward_down_matrix), "sp", (0, 1)
    )

    def to_blocks(tensor):
        return (
            tensor.astype(jnp.float32)
            .reshape(block_count, block_len, head_count, head_dim)
            .transpose(0, 2, 1, 3)
        )

    def gate_block_list(tensor):
        return tensor.reshape(head_count, block_count, block_len).transpose(1, 0, 2)

    query_blk = to_blocks(queries)
    key_blk = to_blocks(memory_keys) * head_dim ** (-0.5)
    val_blk = to_blocks(memory_values)
    gate_blk = gate_block_list(input_preactivation)
    decay_logarithm = jnp.cumsum(
        gate_block_list(jax.nn.log_sigmoid(forget_preactivation) + extra_forget_terms), axis=-1
    )
    summaries = block_summary(key_blk, val_blk, gate_blk, decay_logarithm)
    zero_heads = jnp.zeros((head_count,), jnp.float32)
    zero_memory = jnp.zeros((head_count, head_dim, head_dim), jnp.float32)
    zero_state = (zero_heads, jnp.full((head_count,), neg_big, jnp.float32), zero_memory)
    prefixes = []
    running = zero_state
    for block_idx in range(block_count):
        prefixes.append(running)
        running = combine(running, tuple((member[block_idx] for member in summaries)))
    before = prefix_by_doubling(running, "sp", combine)
    anchor = (zero_heads, zero_heads, zero_memory)
    incoming = combine(anchor, before)
    starts = [combine(incoming, prefix) for prefix in prefixes]
    start_max = jnp.stack([each_state[1] for each_state in starts])
    start_memory = jnp.stack([each_state[2] for each_state in starts])
    causal = lax.broadcasted_iota(jnp.int32, (block_len, block_len), 0) >= lax.broadcasted_iota(
        jnp.int32, (block_len, block_len), 1
    )
    log_weight = (
        decay_logarithm[..., :, None] - decay_logarithm[..., None, :] + gate_blk[..., None, :]
    )
    log_weight = jnp.where(causal, log_weight, neg_big)
    carry_log = decay_logarithm + start_max[..., None]
    row_max = jnp.maximum(jnp.max(log_weight, axis=-1), carry_log)
    scores = jnp.einsum("bhtd,bhsd->bhts", query_blk, key_blk, precision=highest) * jnp.exp(
        log_weight - row_max[..., None]
    )
    carry_scale = jnp.exp(carry_log - row_max)
    hidden = jnp.einsum("bhts,bhsv->bhtv", scores, val_blk, precision=highest)
    hidden = hidden + carry_scale[..., None] * jnp.einsum(
        "bhvk,bhtk->bhtv", start_memory, query_blk, precision=highest
    )
    hidden = hidden.transpose(0, 2, 1, 3).reshape(tok_count, head_count, head_dim)
    gated = rms_norm(hidden, head_norm_gain) * jax.nn.sigmoid(
        output_preactivation.astype(jnp.float32).reshape(tok_count, head_count, head_dim)
    )
    mixed = gated.reshape(tok_count, head_count * head_dim).astype(jnp.bfloat16)
    branch = sum_at_owner(
        jnp.dot(mixed, output_projection_matrix, preferred_element_type=jnp.float32).astype(
            jnp.bfloat16
        ),
        "tp",
        0,
    )
    mid_state = (residual.astype(jnp.float32) + branch).astype(jnp.bfloat16)
    normed = rms_norm(mid_state.astype(jnp.float32), feedforward_norm_gain).astype(jnp.bfloat16)
    normed_all = gather_directly(normed, "tp", 0)
    upward = jnp.dot(normed_all, whole_up, preferred_element_type=jnp.float32)
    active = jnp.square(jax.nn.relu(upward)).astype(jnp.bfloat16)
    mlp_sum = sum_at_owner(
        jnp.dot(active, whole_down, preferred_element_type=jnp.float32).astype(jnp.bfloat16),
        "tp",
        0,
    )
    return (mid_state.astype(jnp.float32) + mlp_sum).astype(jnp.bfloat16)


def solution(mesh):
    in_specs = (
        P(("grp", "sp"), "tp"),
        P(("grp", "sp"), "tp"),
        P(("grp", "sp"), "tp"),
        P(("grp", "sp"), "tp"),
        P("tp", ("grp", "sp")),
        P("tp", ("grp", "sp")),
        P("tp", ("grp", "sp")),
        P(),
        P("tp", None),
        P(("grp", "sp", "tp"), None),
        P(),
        P("sp", "tp"),
        P("tp", "sp"),
    )
    out_specs = P(("grp", "sp", "tp"), None)
    return jax.shard_map(shards, mesh=mesh, in_specs=in_specs, out_specs=out_specs, check_vma=False)
```

```python
import jax
import jax.numpy as jnp
from jax import lax
from jax.experimental import pallas as pl
from jax.experimental.pallas import tpu as pltpu
from jax.sharding import PartitionSpec as P

BLOCK = 128


neg_big = -1e30
norm_eps = 1e-06
highest = lax.Precision.HIGHEST


def gathered_weights(up, down, axis):
    return lax.all_gather(jnp.concatenate([up, down.T], axis=1), axis, axis=0, tiled=True)


def shifted_on(x, axis, distance):
    length = lax.axis_size(axis)
    return lax.ppermute(x, axis, [(k, k + distance) for k in range(length - distance)])


def bf16_parts(x):
    parts = []
    for _ in range(3):
        part = lax.reduce_precision(x, 8, 7)
        parts.append(part.astype(jnp.bfloat16))
        x = x - part
    return parts


def packed(state):
    total, top, memory = state
    rows = bf16_parts(total) + bf16_parts(top)
    rows = jnp.concatenate(rows, axis=1)
    rows = jnp.pad(rows, ((0, 0), (0, 16 - rows.shape[1]), (0, 0)))
    return jnp.concatenate([memory.astype(jnp.bfloat16), rows], axis=1)


def unpacked(both, head_dim, present):
    both = both.astype(jnp.float32)
    total = jnp.sum(both[:, head_dim : head_dim + 3], axis=1, keepdims=True)
    top = jnp.sum(both[:, head_dim + 3 : head_dim + 6], axis=1, keepdims=True)
    return (total, jnp.where(present, top, neg_big), both[:, :head_dim])


def prefix_by_doubling(part, axis):
    place = lax.axis_index(axis)
    length = lax.axis_size(axis)
    head_dim = part[2].shape[-1]
    window, earlier, distance = (part, None, 1)
    while distance < length:
        found = unpacked(shifted_on(packed(window), axis, distance), head_dim, place >= distance)
        earlier = found if earlier is None else combine(found, earlier)
        window = combine(found, window)
        distance *= 2
    return earlier


def turned_by(x, axis, steps):
    length = lax.axis_size(axis)
    return lax.ppermute(x, axis, [(k, (k + steps) % length) for k in range(length)])


def with_partner(x, axis):
    return lax.ppermute(x, axis, [(k, k ^ 1) for k in range(lax.axis_size(axis))])


def in_relative_order(x, axis):
    chips = lax.axis_size(axis) // 2
    place = lax.axis_index(axis)
    chip, core = (place // 2, place % 2)
    blocks = x.reshape(chips, 2, -1, x.shape[-1])
    blocks = jnp.where(core == 0, blocks, blocks[:, ::-1])
    rows = [
        lax.dynamic_index_in_dim(blocks, (chip - d + chips) % chips, 0, False) for d in range(chips)
    ]
    return jnp.concatenate([r[0] for r in rows] + [r[1] for r in rows], axis=0)


def sum_of_relative_rows(kept, sent, axis):
    chips = lax.axis_size(axis) // 2
    found = with_partner(sent, axis)
    both = (kept.astype(jnp.float32) + found.astype(jnp.float32)).astype(jnp.bfloat16)
    blocks = both.reshape(chips, -1, both.shape[-1])
    arrived = {d: turned_by(blocks[d], axis, -2 * d) for d in (2, 1, 3)}
    total = blocks[0].astype(jnp.float32)
    for d in range(1, chips):
        total = total + arrived[d].astype(jnp.float32)
    return total


def relative_rows(x, axis):
    chips = lax.axis_size(axis) // 2
    found = {d: turned_by(x, axis, 2 * d) for d in (2, 1, 3)}
    own = jnp.concatenate([x] + [found[d] for d in range(1, chips)], axis=0)
    return own, with_partner(own, axis)


def rms_norm(tensor, gain_vec):
    mean_sq = jnp.mean(tensor * tensor, axis=-1, keepdims=True)
    return tensor * lax.rsqrt(mean_sq + norm_eps) * gain_vec


def combine(earlier, later):
    total_e, max_e, memory_e = earlier
    total_l, max_l, memory_l = later
    carried = total_l + max_e
    new_max = jnp.maximum(carried, max_l)
    old_part = jnp.exp(carried - new_max)
    new_part = jnp.exp(max_l - new_max)
    return (total_e + total_l, new_max, old_part * memory_e + new_part * memory_l)


def block_prefixes(totals, tops, memories):
    count = totals.shape[0]
    j = lax.broadcasted_iota(jnp.int32, (count + 1, count, count), 0)
    b = lax.broadcasted_iota(jnp.int32, (count + 1, count, count), 1)
    i = lax.broadcasted_iota(jnp.int32, (count + 1, count, count), 2)
    between = ((b < i) & (i < j))[..., None]
    gap = jnp.sum(jnp.where(between, totals[None, None], 0.0), axis=2)
    used = (b < j)[:, :, :1]
    logs = jnp.where(used, gap + tops[None], neg_big)
    top = jnp.max(logs, axis=1)
    scale = jnp.where(used, jnp.exp(logs - top[:, None]), 0.0)
    total = jnp.sum(jnp.where(used, totals[None], 0.0), axis=1)
    memory = jnp.sum(scale[..., None, None] * memories[None], axis=1)
    lanes = (count + 1, totals.shape[1], 1, memories.shape[-1])
    spread = lambda x: jnp.broadcast_to(x[..., None, None], lanes)
    return spread(total), spread(top), memory


def feed_forward_kernel(own_ref, other_ref, up_ref, down_ref, out_ref, active_ref):
    step = pl.program_id(0)
    width = up_ref.shape[1]
    ups = active_ref.shape[1] // width
    half = own_ref.shape[0]

    @pl.when(step < ups)
    def _():
        cols = pl.ds(pl.multiple_of(step * width, width), width)
        for k, rows_ref in enumerate((own_ref, other_ref)):
            upward = jnp.dot(rows_ref[...], up_ref[...], preferred_element_type=jnp.float32)
            active = jnp.square(jnp.maximum(upward, 0.0)).astype(jnp.bfloat16)
            active_ref[k * half : (k + 1) * half, cols] = active

    @pl.when(step >= ups)
    def _():
        out_ref[...] = lax.dot_general(
            active_ref[...],
            down_ref[...],
            (((1,), (1,)), ((), ())),
            preferred_element_type=jnp.float32,
        ).astype(jnp.bfloat16)


def feed_forward(own, other, weights, hidden):
    half, features = own.shape
    up_width, down_height = (hidden // 2, features // 4)
    ups, downs = (hidden // up_width, features // down_height)
    return pl.pallas_call(
        feed_forward_kernel,
        grid=(ups + downs,),
        out_shape=jax.ShapeDtypeStruct((2 * half, features), jnp.bfloat16),
        in_specs=[
            pl.BlockSpec((half, features), lambda i: (0, 0)),
            pl.BlockSpec((half, features), lambda i: (0, 0)),
            pl.BlockSpec((features, up_width), lambda i: (0, jnp.minimum(i, ups - 1))),
            pl.BlockSpec((down_height, hidden), lambda i: (jnp.maximum(i - ups, 0), 1)),
        ],
        out_specs=pl.BlockSpec((2 * half, down_height), lambda i: (0, jnp.maximum(i - ups, 0))),
        scratch_shapes=[pltpu.VMEM((2 * half, hidden), jnp.bfloat16)],
        compiler_params=pltpu.CompilerParams(
            dimension_semantics=("arbitrary",), vmem_limit_bytes=40 * 1024 * 1024
        ),
        cost_estimate=pl.CostEstimate(
            flops=8 * half * features * hidden,
            bytes_accessed=4 * features * hidden + 8 * half * features,
            transcendentals=0,
        ),
        name="feed_forward",
    )(own, other, weights, weights)


def block_summary(key_blk, val_blk, gate_blk, decay_logarithm):
    block_total = decay_logarithm[..., -1]
    tail_log = block_total[..., None] - decay_logarithm + gate_blk
    tail_max = jnp.max(tail_log, axis=-1)
    weights = jnp.exp(tail_log - tail_max[..., None])
    memory = jnp.einsum("bhsv,bhsk->bhvk", weights[..., None] * val_blk, key_blk, precision=highest)
    return (block_total, tail_max, memory)


def shards(
    queries,
    memory_keys,
    memory_values,
    output_preactivation,
    input_preactivation,
    forget_preactivation,
    extra_forget_terms,
    head_norm_gain,
    output_projection_matrix,
    residual,
    feedforward_norm_gain,
    feedforward_up_matrix,
    feedforward_down_matrix,
):
    tok_count = queries.shape[0]
    head_count = input_preactivation.shape[0]
    head_dim = queries.shape[1] // head_count
    block_len = BLOCK
    block_count = tok_count // block_len
    weights = gathered_weights(feedforward_up_matrix, feedforward_down_matrix, "sp")

    def to_blocks(tensor):
        return (
            tensor.astype(jnp.float32)
            .reshape(block_count, block_len, head_count, head_dim)
            .transpose(0, 2, 1, 3)
        )

    def gate_block_list(tensor):
        return tensor.reshape(head_count, block_count, block_len).transpose(1, 0, 2)

    query_blk = to_blocks(queries)
    key_blk = to_blocks(memory_keys) * head_dim ** (-0.5)
    val_blk = to_blocks(memory_values)
    gate_blk = gate_block_list(input_preactivation)
    decay_logarithm = jnp.cumsum(
        gate_block_list(jax.nn.log_sigmoid(forget_preactivation) + extra_forget_terms), axis=-1
    )
    summaries = block_summary(key_blk, val_blk, gate_blk, decay_logarithm)
    prefix_total, prefix_top, prefix_memory = block_prefixes(*summaries)
    whole = (prefix_total[-1], prefix_top[-1], prefix_memory[-1])
    before_total, before_top, before_memory = prefix_by_doubling(whole, "sp")
    incoming_top = jnp.maximum(before_total, before_top)
    incoming_memory = jnp.exp(before_top - incoming_top) * before_memory
    carried = prefix_total[:-1] + incoming_top
    start_top = jnp.maximum(carried, prefix_top[:-1])
    start_memory = (
        jnp.exp(carried - start_top) * incoming_memory
        + jnp.exp(prefix_top[:-1] - start_top) * prefix_memory[:-1]
    )
    start_max = start_top[:, :, 0, 0]
    causal = lax.broadcasted_iota(jnp.int32, (block_len, block_len), 0) >= lax.broadcasted_iota(
        jnp.int32, (block_len, block_len), 1
    )
    log_weight = (
        decay_logarithm[..., :, None] - decay_logarithm[..., None, :] + gate_blk[..., None, :]
    )
    log_weight = jnp.where(causal, log_weight, neg_big)
    carry_log = decay_logarithm + start_max[..., None]
    row_max = jnp.maximum(jnp.max(log_weight, axis=-1), carry_log)
    scores = jnp.einsum("bhtd,bhsd->bhts", query_blk, key_blk, precision=highest) * jnp.exp(
        log_weight - row_max[..., None]
    )
    carry_scale = jnp.exp(carry_log - row_max)
    hidden = jnp.einsum("bhts,bhsv->bhtv", scores, val_blk, precision=highest)
    hidden = hidden + carry_scale[..., None] * jnp.einsum(
        "bhvk,bhtk->bhtv", start_memory, query_blk, precision=highest
    )
    hidden = hidden.transpose(0, 2, 1, 3).reshape(tok_count, head_count, head_dim)
    gated = rms_norm(hidden, head_norm_gain) * jax.nn.sigmoid(
        output_preactivation.astype(jnp.float32).reshape(tok_count, head_count, head_dim)
    )
    mixed = gated.reshape(tok_count, head_count * head_dim).astype(jnp.bfloat16)
    mixed = in_relative_order(mixed, "tp")
    partial_branch = jnp.dot(
        mixed, output_projection_matrix, preferred_element_type=jnp.float32
    ).astype(jnp.bfloat16)
    middle = tok_count // 2
    branch = sum_of_relative_rows(partial_branch[:middle], partial_branch[middle:], "tp")
    mid_state = (residual.astype(jnp.float32) + branch).astype(jnp.bfloat16)
    normed = rms_norm(mid_state.astype(jnp.float32), feedforward_norm_gain).astype(jnp.bfloat16)
    own, other = relative_rows(normed, "tp")
    mlp_rows = feed_forward(own, other, weights, feedforward_up_matrix.shape[1])
    mlp_sum = sum_of_relative_rows(mlp_rows[:middle], mlp_rows[middle:], "tp")
    return (mid_state.astype(jnp.float32) + mlp_sum).astype(jnp.bfloat16)


def solution(mesh):
    in_specs = (
        P(("grp", "sp"), "tp"),
        P(("grp", "sp"), "tp"),
        P(("grp", "sp"), "tp"),
        P(("grp", "sp"), "tp"),
        P("tp", ("grp", "sp")),
        P("tp", ("grp", "sp")),
        P("tp", ("grp", "sp")),
        P(),
        P("tp", None),
        P(("grp", "sp", "tp"), None),
        P(),
        P("sp", "tp"),
        P("tp", "sp"),
    )
    out_specs = P(("grp", "sp", "tp"), None)
    return jax.shard_map(shards, mesh=mesh, in_specs=in_specs, out_specs=out_specs, check_vma=False)
```

```python
import jax
import jax.numpy as jnp
from jax import lax
from jax.experimental import pallas as pl
from jax.experimental.pallas import tpu as pltpu
from jax.sharding import PartitionSpec as P

BLOCK = 128


neg_big = -1e30
norm_eps = 1e-06
highest = lax.Precision.HIGHEST


def gathered_weights(up, down, axis):
    return lax.all_gather(jnp.concatenate([up, down.T], axis=1), axis, axis=0, tiled=True)


def shifted_on(x, axis, distance):
    length = lax.axis_size(axis)
    return lax.ppermute(x, axis, [(k, k + distance) for k in range(length - distance)])


def bf16_parts(x):
    parts = []
    for _ in range(3):
        part = lax.reduce_precision(x, 8, 7)
        parts.append(part.astype(jnp.bfloat16))
        x = x - part
    return parts


def packed(state):
    total, top, memory = state
    rows = bf16_parts(total) + bf16_parts(top)
    rows = jnp.concatenate(rows, axis=1)
    rows = jnp.pad(rows, ((0, 0), (0, 16 - rows.shape[1]), (0, 0)))
    return jnp.concatenate([memory.astype(jnp.bfloat16), rows], axis=1)


def unpacked(both, head_dim, present):
    both = both.astype(jnp.float32)
    total = jnp.sum(both[:, head_dim : head_dim + 3], axis=1, keepdims=True)
    top = jnp.sum(both[:, head_dim + 3 : head_dim + 6], axis=1, keepdims=True)
    return (total, jnp.where(present, top, neg_big), both[:, :head_dim])


def prefix_by_doubling(part, axis):
    place = lax.axis_index(axis)
    length = lax.axis_size(axis)
    head_dim = part[2].shape[-1]
    window, earlier, distance = (part, None, 1)
    while distance < length:
        found = unpacked(shifted_on(packed(window), axis, distance), head_dim, place >= distance)
        earlier = found if earlier is None else combine(found, earlier)
        window = combine(found, window)
        distance *= 2
    return earlier


def with_partner(x, axis):
    return lax.ppermute(x, axis, [(k, k ^ 1) for k in range(lax.axis_size(axis))])


def among_chips(blocks, axis):
    length = lax.axis_size(axis)
    groups = [list(range(core, length, 2)) for core in range(2)]
    return lax.all_to_all(blocks, axis, 0, 0, tiled=True, axis_index_groups=groups)


def own_core_first(x, axis):
    chips = lax.axis_size(axis) // 2
    core = lax.axis_index(axis) % 2
    blocks = x.reshape(chips, 2, -1, x.shape[-1])
    first = jnp.where(core == 0, blocks[:, 0], blocks[:, 1])
    second = jnp.where(core == 0, blocks[:, 1], blocks[:, 0])
    return jnp.concatenate([first, second], axis=0).reshape(x.shape)


def sum_at_owner(rows, axis):
    chips = lax.axis_size(axis) // 2
    half = rows.shape[0] // 2
    found = with_partner(rows[half:], axis)
    both = (rows[:half].astype(jnp.float32) + found.astype(jnp.float32)).astype(jnp.bfloat16)
    blocks = among_chips(both.reshape(chips, -1, both.shape[-1]), axis)
    return jnp.sum(blocks.astype(jnp.float32), axis=0)


def rows_of_all(x, axis):
    chips = lax.axis_size(axis) // 2
    own = among_chips(jnp.broadcast_to(x, (chips, *x.shape)), axis).reshape(-1, x.shape[-1])
    return own, with_partner(own, axis)


def rms_norm(tensor, gain_vec):
    mean_sq = jnp.mean(tensor * tensor, axis=-1, keepdims=True)
    return tensor * lax.rsqrt(mean_sq + norm_eps) * gain_vec


def combine(earlier, later):
    total_e, max_e, memory_e = earlier
    total_l, max_l, memory_l = later
    carried = total_l + max_e
    new_max = jnp.maximum(carried, max_l)
    old_part = jnp.exp(carried - new_max)
    new_part = jnp.exp(max_l - new_max)
    return (total_e + total_l, new_max, old_part * memory_e + new_part * memory_l)


def block_prefixes(totals, tops, memories):
    count = totals.shape[0]
    j = lax.broadcasted_iota(jnp.int32, (count + 1, count, count), 0)
    b = lax.broadcasted_iota(jnp.int32, (count + 1, count, count), 1)
    i = lax.broadcasted_iota(jnp.int32, (count + 1, count, count), 2)
    between = ((b < i) & (i < j))[..., None]
    gap = jnp.sum(jnp.where(between, totals[None, None], 0.0), axis=2)
    used = (b < j)[:, :, :1]
    logs = jnp.where(used, gap + tops[None], neg_big)
    top = jnp.max(logs, axis=1)
    scale = jnp.where(used, jnp.exp(logs - top[:, None]), 0.0)
    total = jnp.sum(jnp.where(used, totals[None], 0.0), axis=1)
    memory = jnp.sum(scale[..., None, None] * memories[None], axis=1)
    lanes = (count + 1, totals.shape[1], 1, memories.shape[-1])
    spread = lambda x: jnp.broadcast_to(x[..., None, None], lanes)
    return (*lax.optimization_barrier((spread(total), spread(top))), memory)


def feed_forward_kernel(own_ref, other_ref, up_ref, down_ref, out_ref, active_ref):
    step = pl.program_id(0)
    width = up_ref.shape[1]
    ups = active_ref.shape[1] // width
    half = own_ref.shape[0]

    @pl.when(step < ups)
    def _():
        cols = pl.ds(pl.multiple_of(step * width, width), width)
        for k, rows_ref in enumerate((own_ref, other_ref)):
            upward = jnp.dot(rows_ref[...], up_ref[...], preferred_element_type=jnp.float32)
            active = jnp.square(jnp.maximum(upward, 0.0)).astype(jnp.bfloat16)
            active_ref[k * half : (k + 1) * half, cols] = active

    @pl.when(step >= ups)
    def _():
        out_ref[...] = lax.dot_general(
            active_ref[...],
            down_ref[...],
            (((1,), (1,)), ((), ())),
            preferred_element_type=jnp.float32,
        ).astype(jnp.bfloat16)


def feed_forward(own, other, weights, hidden):
    half, features = own.shape
    up_width, down_height = (hidden // 2, features // 4)
    ups, downs = (hidden // up_width, features // down_height)
    return pl.pallas_call(
        feed_forward_kernel,
        grid=(ups + downs,),
        out_shape=jax.ShapeDtypeStruct((2 * half, features), jnp.bfloat16),
        in_specs=[
            pl.BlockSpec((half, features), lambda i: (0, 0)),
            pl.BlockSpec((half, features), lambda i: (0, 0)),
            pl.BlockSpec((features, up_width), lambda i: (0, jnp.minimum(i, ups - 1))),
            pl.BlockSpec((down_height, hidden), lambda i: (jnp.maximum(i - ups, 0), 1)),
        ],
        out_specs=pl.BlockSpec((2 * half, down_height), lambda i: (0, jnp.maximum(i - ups, 0))),
        scratch_shapes=[pltpu.VMEM((2 * half, hidden), jnp.bfloat16)],
        compiler_params=pltpu.CompilerParams(
            dimension_semantics=("arbitrary",), vmem_limit_bytes=48 * 1024 * 1024
        ),
        cost_estimate=pl.CostEstimate(
            flops=8 * half * features * hidden,
            bytes_accessed=4 * features * hidden + 8 * half * features,
            transcendentals=0,
        ),
        name="feed_forward",
    )(own, other, weights, weights)


def block_summary(key_blk, val_blk, gate_blk, decay_logarithm):
    block_total = decay_logarithm[..., -1]
    tail_log = block_total[..., None] - decay_logarithm + gate_blk
    tail_max = jnp.max(tail_log, axis=-1)
    weights = jnp.exp(tail_log - tail_max[..., None])
    memory = jnp.einsum("bhsv,bhsk->bhvk", weights[..., None] * val_blk, key_blk, precision=highest)
    return (block_total, tail_max, memory)


def shards(
    queries,
    memory_keys,
    memory_values,
    output_preactivation,
    input_preactivation,
    forget_preactivation,
    extra_forget_terms,
    head_norm_gain,
    output_projection_matrix,
    residual,
    feedforward_norm_gain,
    feedforward_up_matrix,
    feedforward_down_matrix,
):
    tok_count = queries.shape[0]
    head_count = input_preactivation.shape[0]
    head_dim = queries.shape[1] // head_count
    block_len = BLOCK
    block_count = tok_count // block_len
    weights = gathered_weights(feedforward_up_matrix, feedforward_down_matrix, "sp")

    def to_blocks(tensor):
        return (
            tensor.astype(jnp.float32)
            .reshape(block_count, block_len, head_count, head_dim)
            .transpose(0, 2, 1, 3)
        )

    def gate_block_list(tensor):
        return tensor.reshape(head_count, block_count, block_len).transpose(1, 0, 2)

    query_blk = to_blocks(queries)
    key_blk = to_blocks(memory_keys) * head_dim ** (-0.5)
    val_blk = to_blocks(memory_values)
    gate_blk = gate_block_list(input_preactivation)
    decay_logarithm = jnp.cumsum(
        gate_block_list(jax.nn.log_sigmoid(forget_preactivation) + extra_forget_terms), axis=-1
    )
    summaries = block_summary(key_blk, val_blk, gate_blk, decay_logarithm)
    prefix_total, prefix_top, prefix_memory = block_prefixes(*summaries)
    whole = (prefix_total[-1], prefix_top[-1], prefix_memory[-1])
    before_total, before_top, before_memory = prefix_by_doubling(whole, "sp")
    incoming_top = jnp.maximum(before_total, before_top)
    incoming_memory = jnp.exp(before_top - incoming_top) * before_memory
    carried = prefix_total[:-1] + incoming_top
    start_top = jnp.maximum(carried, prefix_top[:-1])
    start_memory = (
        jnp.exp(carried - start_top) * incoming_memory
        + jnp.exp(prefix_top[:-1] - start_top) * prefix_memory[:-1]
    )
    start_max = start_top[:, :, 0, 0]
    causal = lax.broadcasted_iota(jnp.int32, (block_len, block_len), 0) >= lax.broadcasted_iota(
        jnp.int32, (block_len, block_len), 1
    )
    log_weight = (
        decay_logarithm[..., :, None] - decay_logarithm[..., None, :] + gate_blk[..., None, :]
    )
    log_weight = jnp.where(causal, log_weight, neg_big)
    carry_log = decay_logarithm + start_max[..., None]
    row_max = jnp.maximum(jnp.max(log_weight, axis=-1), carry_log)
    scores = jnp.einsum("bhtd,bhsd->bhts", query_blk, key_blk, precision=highest) * jnp.exp(
        log_weight - row_max[..., None]
    )
    carry_scale = jnp.exp(carry_log - row_max)
    hidden = jnp.einsum("bhts,bhsv->bhtv", scores, val_blk, precision=highest)
    hidden = hidden + carry_scale[..., None] * jnp.einsum(
        "bhvk,bhtk->bhtv", start_memory, query_blk, precision=highest
    )
    hidden = hidden.transpose(0, 2, 1, 3).reshape(tok_count, head_count, head_dim)
    gated = rms_norm(hidden, head_norm_gain) * jax.nn.sigmoid(
        output_preactivation.astype(jnp.float32).reshape(tok_count, head_count, head_dim)
    )
    mixed = gated.reshape(tok_count, head_count * head_dim).astype(jnp.bfloat16)
    mixed = own_core_first(mixed, "tp")
    partial_branch = jnp.dot(
        mixed, output_projection_matrix, preferred_element_type=jnp.float32
    ).astype(jnp.bfloat16)
    branch = sum_at_owner(partial_branch, "tp")
    mid_state = (residual.astype(jnp.float32) + branch).astype(jnp.bfloat16)
    normed = rms_norm(mid_state.astype(jnp.float32), feedforward_norm_gain).astype(jnp.bfloat16)
    own, other = rows_of_all(normed, "tp")
    mlp_rows = feed_forward(own, other, weights, feedforward_up_matrix.shape[1])
    mlp_sum = sum_at_owner(mlp_rows, "tp")
    return (mid_state.astype(jnp.float32) + mlp_sum).astype(jnp.bfloat16)


def solution(mesh):
    in_specs = (
        P(("grp", "sp"), "tp"),
        P(("grp", "sp"), "tp"),
        P(("grp", "sp"), "tp"),
        P(("grp", "sp"), "tp"),
        P("tp", ("grp", "sp")),
        P("tp", ("grp", "sp")),
        P("tp", ("grp", "sp")),
        P(),
        P("tp", None),
        P(("grp", "sp", "tp"), None),
        P(),
        P("sp", "tp"),
        P("tp", "sp"),
    )
    out_specs = P(("grp", "sp", "tp"), None)
    return jax.shard_map(shards, mesh=mesh, in_specs=in_specs, out_specs=out_specs, check_vma=False)
```

```python
import functools
import jax
import jax.numpy as jnp
import numpy as np
from jax import lax
from jax.experimental import pallas as pl
from jax.experimental.pallas import tpu as pltpu
from jax.sharding import Mesh, PartitionSpec as P

BLOCK = 128


neg_big = -1e30
norm_eps = 1e-06
highest = lax.Precision.HIGHEST


def gathered_weights(up, down):
    both = jnp.concatenate([up, down.T], axis=1)
    whole = lax.all_gather(both, ("sp", "core"), axis=0, tiled=True)
    return whole.reshape(lax.axis_size("sp"), lax.axis_size("core"), *both.shape)


def shifted_on(x, axis, distance):
    length = lax.axis_size(axis)
    return lax.ppermute(x, axis, [(k, k + distance) for k in range(length - distance)])


def bf16_parts(x):
    parts = []
    for _ in range(3):
        part = lax.reduce_precision(x, 8, 7)
        parts.append(part.astype(jnp.bfloat16))
        x = x - part
    return parts


def packed(state):
    total, top, memory = state
    rows = bf16_parts(total) + bf16_parts(top)
    rows = jnp.concatenate(rows, axis=1)
    rows = jnp.pad(rows, ((0, 0), (0, 16 - rows.shape[1]), (0, 0)))
    return jnp.concatenate([memory.astype(jnp.bfloat16), rows], axis=1)


def unpacked(both, head_dim, present):
    both = both.astype(jnp.float32)
    total = jnp.sum(both[:, head_dim : head_dim + 3], axis=1, keepdims=True)
    top = jnp.sum(both[:, head_dim + 3 : head_dim + 6], axis=1, keepdims=True)
    return (total, jnp.where(present, top, neg_big), both[:, :head_dim])


def prefix_by_doubling(part, axis):
    place = lax.axis_index(axis)
    length = lax.axis_size(axis)
    head_dim = part[2].shape[-1]
    window, earlier, distance = (part, None, 1)
    while distance < length:
        found = unpacked(shifted_on(packed(window), axis, distance), head_dim, place >= distance)
        earlier = found if earlier is None else combine(found, earlier)
        window = combine(found, window)
        distance *= 2
    return earlier


def among_chips(blocks):
    return lax.all_to_all(blocks, "chip", 0, 0, tiled=True)


def own_core_first(x):
    chips = lax.axis_size("chip")
    core = lax.axis_index("core")
    blocks = x.reshape(chips, 2, -1, x.shape[-1])
    first = jnp.where(core == 0, blocks[:, 0], blocks[:, 1])
    second = jnp.where(core == 0, blocks[:, 1], blocks[:, 0])
    return jnp.concatenate([first, second], axis=0).reshape(x.shape)


def sum_of_cores(rows):
    half = rows.shape[0] // 2
    found = lax.ppermute(rows[half:], "core", [(0, 1), (1, 0)])
    return (rows[:half].astype(jnp.float32) + found.astype(jnp.float32)).astype(jnp.bfloat16)


def sum_of_chips(rows):
    blocks = among_chips(rows.reshape(lax.axis_size("chip"), -1, rows.shape[-1]))
    return jnp.sum(blocks.astype(jnp.float32), axis=0)


def rows_of_chips(x):
    copies = jnp.broadcast_to(x, (lax.axis_size("chip"), *x.shape))
    return among_chips(copies).reshape(-1, x.shape[-1])


def rms_norm(tensor, gain_vec):
    mean_sq = jnp.mean(tensor * tensor, axis=-1, keepdims=True)
    return tensor * lax.rsqrt(mean_sq + norm_eps) * gain_vec


def combine(earlier, later):
    total_e, max_e, memory_e = earlier
    total_l, max_l, memory_l = later
    carried = total_l + max_e
    new_max = jnp.maximum(carried, max_l)
    old_part = jnp.exp(carried - new_max)
    new_part = jnp.exp(max_l - new_max)
    return (total_e + total_l, new_max, old_part * memory_e + new_part * memory_l)


def block_prefixes(totals, tops, memories):
    count = totals.shape[0]
    j = lax.broadcasted_iota(jnp.int32, (count + 1, count, count), 0)
    b = lax.broadcasted_iota(jnp.int32, (count + 1, count, count), 1)
    i = lax.broadcasted_iota(jnp.int32, (count + 1, count, count), 2)
    between = ((b < i) & (i < j))[..., None]
    gap = jnp.sum(jnp.where(between, totals[None, None], 0.0), axis=2)
    used = (b < j)[:, :, :1]
    logs = jnp.where(used, gap + tops[None], neg_big)
    top = jnp.max(logs, axis=1)
    scale = jnp.where(used, jnp.exp(logs - top[:, None]), 0.0)
    total = jnp.sum(jnp.where(used, totals[None], 0.0), axis=1)
    memory = jnp.sum(scale[..., None, None] * memories[None], axis=1)
    lanes = (count + 1, totals.shape[1], 1, memories.shape[-1])
    spread = lambda x: jnp.broadcast_to(x[..., None, None], lanes)
    return (*lax.optimization_barrier((spread(total), spread(top))), memory)


def feed_forward_kernel(ups, rows_ref, up_ref, down_ref, out_ref, active_ref):
    step = pl.program_id(0)
    width = up_ref.shape[-1]
    hidden = down_ref.shape[-1]

    @pl.when(step < ups)
    def _():
        cols = pl.ds(pl.multiple_of(step * width, width), width)
        upward = jnp.dot(
            rows_ref[...], up_ref[...].reshape(-1, width), preferred_element_type=jnp.float32
        )
        active_ref[:, cols] = jnp.square(jnp.maximum(upward, 0.0)).astype(jnp.bfloat16)

    @pl.when(step >= ups)
    def _():
        total = None
        for core in range(down_ref.shape[1]):
            part = lax.dot_general(
                active_ref[:, core * hidden : (core + 1) * hidden],
                down_ref[:, core].reshape(-1, hidden),
                (((1,), (1,)), ((), ())),
                preferred_element_type=jnp.float32,
            )
            total = part if total is None else total + part
        out_ref[...] = total.astype(jnp.bfloat16)


def feed_forward(rows, weights, hidden):
    count, features = rows.shape
    pieces, cores, height, _ = weights.shape
    width, taken = (hidden, pieces // 2)
    each = hidden // width
    ups, downs = (cores * each, pieces // taken)
    up_at = lambda i: jnp.minimum(i, ups - 1)
    down_at = lambda i: jnp.maximum(i - ups, 0)
    return pl.pallas_call(
        functools.partial(feed_forward_kernel, ups),
        grid=(ups + downs,),
        out_shape=jax.ShapeDtypeStruct((count, features), jnp.bfloat16),
        in_specs=[
            pl.BlockSpec((count, features), lambda i: (0, 0)),
            pl.BlockSpec(
                (pieces, 1, height, width), lambda i: (0, up_at(i) // each, 0, up_at(i) % each)
            ),
            pl.BlockSpec((taken, cores, height, hidden), lambda i: (down_at(i), 0, 0, 1)),
        ],
        out_specs=pl.BlockSpec((count, taken * height), lambda i: (0, down_at(i))),
        scratch_shapes=[pltpu.VMEM((count, cores * hidden), jnp.bfloat16)],
        compiler_params=pltpu.CompilerParams(
            dimension_semantics=("arbitrary",), vmem_limit_bytes=48 * 1024 * 1024
        ),
        cost_estimate=pl.CostEstimate(
            flops=4 * count * features * cores * hidden,
            bytes_accessed=4 * features * cores * hidden + 4 * count * features,
            transcendentals=0,
        ),
        name="feed_forward",
    )(rows, weights, weights)


def block_summary(key_blk, val_blk, gate_blk, decay_logarithm):
    block_total = decay_logarithm[..., -1]
    tail_log = block_total[..., None] - decay_logarithm + gate_blk
    tail_max = jnp.max(tail_log, axis=-1)
    weights = jnp.exp(tail_log - tail_max[..., None])
    memory = jnp.einsum("bhsv,bhsk->bhvk", weights[..., None] * val_blk, key_blk, precision=highest)
    return (block_total, tail_max, memory)


def shards(
    queries,
    memory_keys,
    memory_values,
    output_preactivation,
    input_preactivation,
    forget_preactivation,
    extra_forget_terms,
    head_norm_gain,
    output_projection_matrix,
    residual,
    feedforward_norm_gain,
    feedforward_up_matrix,
    feedforward_down_matrix,
):
    tok_count = queries.shape[0]
    head_count = input_preactivation.shape[0]
    head_dim = queries.shape[1] // head_count
    block_len = BLOCK
    block_count = tok_count // block_len
    weights = gathered_weights(feedforward_up_matrix, feedforward_down_matrix)

    def to_blocks(tensor):
        return (
            tensor.astype(jnp.float32)
            .reshape(block_count, block_len, head_count, head_dim)
            .transpose(0, 2, 1, 3)
        )

    def gate_block_list(tensor):
        return tensor.reshape(head_count, block_count, block_len).transpose(1, 0, 2)

    query_blk = to_blocks(queries)
    key_blk = to_blocks(memory_keys) * head_dim ** (-0.5)
    val_blk = to_blocks(memory_values)
    gate_blk = gate_block_list(input_preactivation)
    decay_logarithm = jnp.cumsum(
        gate_block_list(jax.nn.log_sigmoid(forget_preactivation) + extra_forget_terms), axis=-1
    )
    summaries = block_summary(key_blk, val_blk, gate_blk, decay_logarithm)
    prefix_total, prefix_top, prefix_memory = block_prefixes(*summaries)
    whole = (prefix_total[-1], prefix_top[-1], prefix_memory[-1])
    before_total, before_top, before_memory = prefix_by_doubling(whole, "sp")
    incoming_top = jnp.maximum(before_total, before_top)
    incoming_memory = jnp.exp(before_top - incoming_top) * before_memory
    carried = prefix_total[:-1] + incoming_top
    start_top = jnp.maximum(carried, prefix_top[:-1])
    start_memory = (
        jnp.exp(carried - start_top) * incoming_memory
        + jnp.exp(prefix_top[:-1] - start_top) * prefix_memory[:-1]
    )
    start_max = start_top[:, :, 0, 0]
    causal = lax.broadcasted_iota(jnp.int32, (block_len, block_len), 0) >= lax.broadcasted_iota(
        jnp.int32, (block_len, block_len), 1
    )
    log_weight = (
        decay_logarithm[..., :, None] - decay_logarithm[..., None, :] + gate_blk[..., None, :]
    )
    log_weight = jnp.where(causal, log_weight, neg_big)
    carry_log = decay_logarithm + start_max[..., None]
    row_max = jnp.maximum(jnp.max(log_weight, axis=-1), carry_log)
    scores = jnp.einsum("bhtd,bhsd->bhts", query_blk, key_blk, precision=highest) * jnp.exp(
        log_weight - row_max[..., None]
    )
    carry_scale = jnp.exp(carry_log - row_max)
    hidden = jnp.einsum("bhts,bhsv->bhtv", scores, val_blk, precision=highest)
    hidden = hidden + carry_scale[..., None] * jnp.einsum(
        "bhvk,bhtk->bhtv", start_memory, query_blk, precision=highest
    )
    hidden = hidden.transpose(0, 2, 1, 3).reshape(tok_count, head_count, head_dim)
    gated = rms_norm(hidden, head_norm_gain) * jax.nn.sigmoid(
        output_preactivation.astype(jnp.float32).reshape(tok_count, head_count, head_dim)
    )
    mixed = gated.reshape(tok_count, head_count * head_dim).astype(jnp.bfloat16)
    mixed = own_core_first(mixed)
    partial_branch = jnp.dot(
        mixed, output_projection_matrix, preferred_element_type=jnp.float32
    ).astype(jnp.bfloat16)
    branch = sum_of_chips(sum_of_cores(partial_branch))
    mid_state = (residual.astype(jnp.float32) + branch).astype(jnp.bfloat16)
    normed = rms_norm(mid_state.astype(jnp.float32), feedforward_norm_gain).astype(jnp.bfloat16)
    mlp_rows = feed_forward(rows_of_chips(normed), weights, feedforward_up_matrix.shape[1])
    return (mid_state.astype(jnp.float32) + sum_of_chips(mlp_rows)).astype(jnp.bfloat16)


def solution(mesh):
    groups, places, lanes = mesh.devices.shape
    split = Mesh(
        np.asarray(mesh.devices).reshape(groups, places, lanes // 2, 2),
        ("grp", "sp", "chip", "core"),
    )
    rows, heads = (("grp", "sp"), ("chip", "core"))
    in_specs = (
        P(rows, heads),
        P(rows, heads),
        P(rows, heads),
        P(rows, heads),
        P(heads, rows),
        P(heads, rows),
        P(heads, rows),
        P(),
        P(heads, None),
        P((*rows, *heads), None),
        P(),
        P("sp", heads),
        P(heads, "sp"),
    )
    out_specs = P((*rows, *heads), None)
    return jax.shard_map(
        shards, mesh=split, in_specs=in_specs, out_specs=out_specs, check_vma=False
    )
```

```python
import functools
import jax
import jax.numpy as jnp
import numpy as np
from jax import lax
from jax.experimental import pallas as pl
from jax.experimental.pallas import tpu as pltpu
from jax.sharding import Mesh, PartitionSpec as P

BLOCK = 128


neg_big = -1e30
norm_eps = 1e-06
highest = lax.Precision.HIGHEST


def gathered_weights(up, down):
    both = jnp.concatenate([up, down.T], axis=1)
    whole = lax.all_gather(both, ("sp", "core"), axis=0, tiled=True)
    return whole.reshape(lax.axis_size("sp"), lax.axis_size("core"), *both.shape)


def bf16_parts(x):
    parts = []
    for _ in range(3):
        part = lax.reduce_precision(x, 8, 7)
        parts.append(part.astype(jnp.bfloat16))
        x = x - part
    return parts


def packed(state):
    total, top, memory = state
    rows = bf16_parts(total) + bf16_parts(top)
    rows = jnp.concatenate(rows, axis=1)
    rows = jnp.pad(rows, ((0, 0), (0, 16 - rows.shape[1]), (0, 0)))
    return jnp.concatenate([memory.astype(jnp.bfloat16), rows], axis=1)


def unpacked(both, head_dim, present):
    both = both.astype(jnp.float32)
    total = jnp.sum(both[:, head_dim : head_dim + 3], axis=1, keepdims=True)
    top = jnp.sum(both[:, head_dim + 3 : head_dim + 6], axis=1, keepdims=True)
    return (total, jnp.where(present, top, neg_big), both[:, :head_dim])


def state_before(part, axis):
    place = lax.axis_index(axis)
    length = lax.axis_size(axis)
    head_dim = part[2].shape[-1]

    def fetched(window, distance, ends):
        pairs = [(end - distance, end) for end in ends]
        stride = ends[1] - ends[0] if len(ends) > 1 else length
        present = (place >= ends[0]) & (lax.rem(place - ends[0] + length, stride) == 0)
        return unpacked(lax.ppermute(packed(window), axis, pairs), head_dim, present)

    window, distance = (part, 1)
    while 2 * distance < length:
        ends = list(range(2 * distance - 1, length, 2 * distance))
        window = combine(fetched(window, distance, ends), window)
        distance *= 2
    distance //= 2
    while distance >= 1:
        ends = list(range(3 * distance - 1, length, 2 * distance))
        window = combine(fetched(window, distance, ends), window)
        distance //= 2
    return fetched(window, 1, list(range(1, length)))


def among_chips(blocks):
    return lax.all_to_all(blocks, "chip", 0, 0, tiled=True)


def own_core_first(x):
    chips = lax.axis_size("chip")
    core = lax.axis_index("core")
    blocks = x.reshape(chips, 2, -1, x.shape[-1])
    first = jnp.where(core == 0, blocks[:, 0], blocks[:, 1])
    second = jnp.where(core == 0, blocks[:, 1], blocks[:, 0])
    return jnp.concatenate([first, second], axis=0).reshape(x.shape)


def sum_of_cores(rows):
    half = rows.shape[0] // 2
    found = lax.ppermute(rows[half:], "core", [(0, 1), (1, 0)])
    return (rows[:half].astype(jnp.float32) + found.astype(jnp.float32)).astype(jnp.bfloat16)


def sum_of_chips(rows):
    blocks = among_chips(rows.reshape(lax.axis_size("chip"), -1, rows.shape[-1]))
    return jnp.sum(blocks.astype(jnp.float32), axis=0)


def rows_of_chips(x):
    copies = jnp.broadcast_to(x, (lax.axis_size("chip"), *x.shape))
    return among_chips(copies).reshape(-1, x.shape[-1])


def rms_norm(tensor, gain_vec):
    mean_sq = jnp.mean(tensor * tensor, axis=-1, keepdims=True)
    return tensor * lax.rsqrt(mean_sq + norm_eps) * gain_vec


def combine(earlier, later):
    total_e, max_e, memory_e = earlier
    total_l, max_l, memory_l = later
    carried = total_l + max_e
    new_max = jnp.maximum(carried, max_l)
    old_part = jnp.exp(carried - new_max)
    new_part = jnp.exp(max_l - new_max)
    return (total_e + total_l, new_max, old_part * memory_e + new_part * memory_l)


def block_prefixes(totals, tops, memories):
    count = totals.shape[0]
    j = lax.broadcasted_iota(jnp.int32, (count + 1, count, count), 0)
    b = lax.broadcasted_iota(jnp.int32, (count + 1, count, count), 1)
    i = lax.broadcasted_iota(jnp.int32, (count + 1, count, count), 2)
    between = ((b < i) & (i < j))[..., None]
    gap = jnp.sum(jnp.where(between, totals[None, None], 0.0), axis=2)
    used = (b < j)[:, :, :1]
    logs = jnp.where(used, gap + tops[None], neg_big)
    top = jnp.max(logs, axis=1)
    scale = jnp.where(used, jnp.exp(logs - top[:, None]), 0.0)
    total = jnp.sum(jnp.where(used, totals[None], 0.0), axis=1)
    memory = jnp.sum(scale[..., None, None] * memories[None], axis=1)
    lanes = (count + 1, totals.shape[1], 1, memories.shape[-1])
    spread = lambda x: jnp.broadcast_to(x[..., None, None], lanes)
    return (*lax.optimization_barrier((spread(total), spread(top))), memory)


def feed_forward_kernel(hidden, rows_ref, weights_ref, out_ref, up_buf, down_buf, active_ref, sems):
    pieces, height, width = up_buf.shape[1:]
    taken, cores = down_buf.shape[1:3]
    ups, downs = (up_buf.shape[0], down_buf.shape[0])
    each = hidden // width
    copies = [
        pltpu.make_async_copy(
            weights_ref.at[:, k // each, :, pl.ds(k % each * width, width)],
            up_buf.at[k],
            sems.at[k],
        )
        for k in range(ups)
    ] + [
        pltpu.make_async_copy(
            weights_ref.at[pl.ds(k * taken, taken), :, :, pl.ds(hidden, hidden)],
            down_buf.at[k],
            sems.at[ups + k],
        )
        for k in range(downs)
    ]
    for copy in copies:
        copy.start()
    rows = rows_ref[...]
    for k in range(ups):
        copies[k].wait()
        upward = jnp.dot(
            rows, up_buf[k].reshape(-1, width), preferred_element_type=jnp.float32
        )
        active = jnp.square(jnp.maximum(upward, 0.0)).astype(jnp.bfloat16)
        active_ref[:, k * width : (k + 1) * width] = active
    for k in range(downs):
        copies[ups + k].wait()
        total = None
        for core in range(cores):
            part = lax.dot_general(
                active_ref[:, core * hidden : (core + 1) * hidden],
                down_buf[k, :, core].reshape(-1, hidden),
                (((1,), (1,)), ((), ())),
                preferred_element_type=jnp.float32,
            )
            total = part if total is None else total + part
        out_ref[:, k * taken * height : (k + 1) * taken * height] = total.astype(jnp.bfloat16)


def feed_forward(rows, weights, hidden):
    count, features = rows.shape
    pieces, cores, height, _ = weights.shape
    width, taken = (hidden // 2, pieces // 4)
    ups, downs = (cores * hidden // width, pieces // taken)
    return pl.pallas_call(
        functools.partial(feed_forward_kernel, hidden),
        out_shape=jax.ShapeDtypeStruct((count, features), jnp.bfloat16),
        in_specs=[
            pl.BlockSpec(memory_space=pltpu.VMEM),
            pl.BlockSpec(memory_space=pl.ANY),
        ],
        out_specs=pl.BlockSpec(memory_space=pltpu.VMEM),
        scratch_shapes=[
            pltpu.VMEM((ups, pieces, height, width), jnp.bfloat16),
            pltpu.VMEM((downs, taken, cores, height, hidden), jnp.bfloat16),
            pltpu.VMEM((count, cores * hidden), jnp.bfloat16),
            pltpu.SemaphoreType.DMA((ups + downs,)),
        ],
        compiler_params=pltpu.CompilerParams(vmem_limit_bytes=48 * 1024 * 1024),
        cost_estimate=pl.CostEstimate(
            flops=4 * count * features * cores * hidden,
            bytes_accessed=4 * features * cores * hidden + 4 * count * features,
            transcendentals=0,
        ),
        name="feed_forward",
    )(rows, weights)


def block_summary(key_blk, val_blk, gate_blk, decay_logarithm):
    block_total = decay_logarithm[..., -1]
    tail_log = block_total[..., None] - decay_logarithm + gate_blk
    tail_max = jnp.max(tail_log, axis=-1)
    weights = jnp.exp(tail_log - tail_max[..., None])
    memory = jnp.einsum("bhsv,bhsk->bhvk", weights[..., None] * val_blk, key_blk, precision=highest)
    return (block_total, tail_max, memory)


def shards(
    queries,
    memory_keys,
    memory_values,
    output_preactivation,
    input_preactivation,
    forget_preactivation,
    extra_forget_terms,
    head_norm_gain,
    output_projection_matrix,
    residual,
    feedforward_norm_gain,
    feedforward_up_matrix,
    feedforward_down_matrix,
):
    tok_count = queries.shape[0]
    head_count = input_preactivation.shape[0]
    head_dim = queries.shape[1] // head_count
    block_len = BLOCK
    block_count = tok_count // block_len
    weights = gathered_weights(feedforward_up_matrix, feedforward_down_matrix)

    def to_blocks(tensor):
        return (
            tensor.astype(jnp.float32)
            .reshape(block_count, block_len, head_count, head_dim)
            .transpose(0, 2, 1, 3)
        )

    def gate_block_list(tensor):
        return tensor.reshape(head_count, block_count, block_len).transpose(1, 0, 2)

    query_blk = to_blocks(queries)
    key_blk = to_blocks(memory_keys) * head_dim ** (-0.5)
    val_blk = to_blocks(memory_values)
    gate_blk = gate_block_list(input_preactivation)
    decay_logarithm = jnp.cumsum(
        gate_block_list(jax.nn.log_sigmoid(forget_preactivation) + extra_forget_terms), axis=-1
    )
    summaries = block_summary(key_blk, val_blk, gate_blk, decay_logarithm)
    prefix_total, prefix_top, prefix_memory = block_prefixes(*summaries)
    whole = (prefix_total[-1], prefix_top[-1], prefix_memory[-1])
    before_total, before_top, before_memory = state_before(whole, "sp")
    incoming_top = jnp.maximum(before_total, before_top)
    incoming_memory = jnp.exp(before_top - incoming_top) * before_memory
    carried = prefix_total[:-1] + incoming_top
    start_top = jnp.maximum(carried, prefix_top[:-1])
    start_memory = (
        jnp.exp(carried - start_top) * incoming_memory
        + jnp.exp(prefix_top[:-1] - start_top) * prefix_memory[:-1]
    )
    start_max = start_top[:, :, 0, 0]
    causal = lax.broadcasted_iota(jnp.int32, (block_len, block_len), 0) >= lax.broadcasted_iota(
        jnp.int32, (block_len, block_len), 1
    )
    log_weight = (
        decay_logarithm[..., :, None] - decay_logarithm[..., None, :] + gate_blk[..., None, :]
    )
    log_weight = jnp.where(causal, log_weight, neg_big)
    carry_log = decay_logarithm + start_max[..., None]
    row_max = jnp.maximum(jnp.max(log_weight, axis=-1), carry_log)
    scores = jnp.einsum("bhtd,bhsd->bhts", query_blk, key_blk, precision=highest) * jnp.exp(
        log_weight - row_max[..., None]
    )
    carry_scale = jnp.exp(carry_log - row_max)
    hidden = jnp.einsum("bhts,bhsv->bhtv", scores, val_blk, precision=highest)
    hidden = hidden + carry_scale[..., None] * jnp.einsum(
        "bhvk,bhtk->bhtv", start_memory, query_blk, precision=highest
    )
    hidden = hidden.transpose(0, 2, 1, 3).reshape(tok_count, head_count, head_dim)
    gated = rms_norm(hidden, head_norm_gain) * jax.nn.sigmoid(
        output_preactivation.astype(jnp.float32).reshape(tok_count, head_count, head_dim)
    )
    mixed = gated.reshape(tok_count, head_count * head_dim).astype(jnp.bfloat16)
    mixed = own_core_first(mixed)
    partial_branch = jnp.dot(
        mixed, output_projection_matrix, preferred_element_type=jnp.float32
    ).astype(jnp.bfloat16)
    branch = sum_of_chips(sum_of_cores(partial_branch))
    mid_state = (residual.astype(jnp.float32) + branch).astype(jnp.bfloat16)
    normed = rms_norm(mid_state.astype(jnp.float32), feedforward_norm_gain).astype(jnp.bfloat16)
    mlp_rows = feed_forward(rows_of_chips(normed), weights, feedforward_up_matrix.shape[1])
    return (mid_state.astype(jnp.float32) + sum_of_chips(mlp_rows)).astype(jnp.bfloat16)


def solution(mesh):
    groups, places, lanes = mesh.devices.shape
    split = Mesh(
        np.asarray(mesh.devices).reshape(groups, places, lanes // 2, 2),
        ("grp", "sp", "chip", "core"),
    )
    rows, heads = (("grp", "sp"), ("chip", "core"))
    in_specs = (
        P(rows, heads),
        P(rows, heads),
        P(rows, heads),
        P(rows, heads),
        P(heads, rows),
        P(heads, rows),
        P(heads, rows),
        P(),
        P(heads, None),
        P((*rows, *heads), None),
        P(),
        P("sp", heads),
        P(heads, "sp"),
    )
    out_specs = P((*rows, *heads), None)
    return jax.shard_map(
        shards, mesh=split, in_specs=in_specs, out_specs=out_specs, check_vma=False
    )
```
